32 devices in a mesh: ep: 8 (over z, x), tp: 4 (over y, core).
Axes of the slice: x: 2, y: 2, z: 4, core: 2. Of those that a mesh axis runs over, the one named last changes fastest.
Arguments:
- tokens: bfloat16 [2048, 2048], P('ep')
- norm_gain: float32 [2048], replicated, may hold values from 0.1 to 1.9
- chosen: int32 [8, 256], replicated, may hold values from 0 to 2047, as said below
- route_weight: float32 [8, 256], P('ep'), may hold values from 0.2 to 1
- gate_weight: bfloat16 [8, 2048, 4096], P('ep', None, 'tp'), may hold values from -0.125 to 0.125
- up_weight: bfloat16 [8, 2048, 4096], P('ep', None, 'tp'), may hold values from -0.125 to 0.125
- down_weight: bfloat16 [8, 4096, 2048], P('ep', 'tp'), may hold values from -0.09375 to 0.09375
Outputs:
- combined: bfloat16 [2048, 2048], P('ep', 'tp')
The draws below stay inside these ranges and needn't reach their ends.
Inputs may be any that keep to these rules, and one draw needn't show every extreme that they name: Each row of chosen lists 256 distinct token numbers in ascending order. Of the 256 consecutive tokens of one index of ep, a row holds at most 48, and every draw has rows that hold exactly 48 of them.
All inputs are finite; a program needn't handle non-finite values.
Results may differ from the reference program's by a relative error of at most 0.02.
Values may be sent and summed in bfloat16 or wider, within the bound.
A program may use at most 64 MiB of HBM per device.

```python
import math
import jax
import jax.numpy as jnp
from jax import lax

D = 2048
FF = 4096
TOK_DEV = 256
EXPERTS = 8
TOKENS = 2048
CAP = 256
FF_BLK = 1024
N_TP = 4


def draw_tokens(key, part):
    keys = jax.random.split(jax.random.fold_in(key, 11), 3)
    row_scale = jnp.exp(jax.random.uniform(keys[0], (TOKENS, 1), jnp.float32, 0.0, math.log(10.0)))
    col_scale = jnp.exp(jax.random.uniform(keys[1], (1, D), jnp.float32, 0.0, math.log(10.0)))
    values = jax.random.normal(keys[2], (TOKENS, D), jnp.float32)
    return (values * row_scale * col_scale / 3.0).astype(jnp.bfloat16)


def draw_chosen(key, part):
    share = TOK_DEV // 8
    pairs = EXPERTS // 2
    steps = jnp.arange(pairs, dtype=jnp.int32)
    spread = share // 2 * steps // max(pairs - 1, 1)
    base = jnp.stack([share + spread, share - spread], axis=1).reshape(EXPERTS)
    expert_keys = jax.random.split(jax.random.fold_in(key, 23), EXPERTS)

    def one_expert(expert_key):
        order_key, rank_key = jax.random.split(expert_key)
        counts = base[jax.random.permutation(order_key, EXPERTS)]
        block_keys = jax.random.split(rank_key, EXPERTS)
        ranks = jax.vmap(lambda block_key: jax.random.permutation(block_key, TOK_DEV))(block_keys)
        picked = (ranks < counts[:, None]).reshape(TOKENS).astype(jnp.int32)
        order = jnp.argsort(1 - picked, stable=True)
        return order[:CAP].astype(jnp.int32)
    return jax.vmap(one_expert)(expert_keys)


def steps_of(stream_key, extent, cuts, least, top_value):
    def one(dim, blocks):
        heights = jax.random.uniform(jax.random.fold_in(jax.random.fold_in(stream_key, 6), dim), (blocks,), jnp.float32, least / len(cuts), top_value / len(cuts))
        return jnp.repeat(jnp.exp(heights), extent[dim] // blocks).reshape((-1,) + (1,) * (len(extent) - dim - 1))

    gain = one(*cuts[0])
    for cut in cuts[1:]:
        gain = gain * one(*cut)
    return gain


def scatter_about(stream_key, shape, width, reach, pieces=(), kind=jnp.bfloat16):
    array = width * jax.random.normal(stream_key, shape, jnp.float32)
    if pieces:
        array = array * steps_of(stream_key, shape, pieces, -0.22, 0.18)
    return jnp.clip(array, -reach, reach).astype(kind)


def setup_inputs(seed: int = 0) -> dict:
    key_list = jax.random.split(jax.random.key(seed), 8)
    return {
        "tokens": draw_tokens(jax.random.fold_in(key_list[7], 71), 0),
        "norm_gain": jnp.clip(1.0 + 0.18 * jax.random.normal(key_list[1], (D,), jnp.float32), 0.1, 1.9),
        "chosen": draw_chosen(jax.random.fold_in(key_list[7], 71), 0),
        "route_weight": jnp.clip(0.2 + 0.8 * jax.random.uniform(key_list[3], (EXPERTS, CAP), jnp.float32) ** steps_of(key_list[3], (EXPERTS, CAP), ((0, 8),), -0.2, 0.2), 0.2, 1.0),
        "gate_weight": scatter_about(key_list[4], (EXPERTS, D, FF), D ** -0.5, 0.125, ((0, 8), (2, 4))),
        "up_weight": scatter_about(key_list[5], (EXPERTS, D, FF), D ** -0.5, 0.125, ((0, 8), (2, 4))),
        "down_weight": scatter_about(key_list[6], (EXPERTS, FF, D), FF ** -0.5, 0.09375, ((0, 8), (1, 4))),
    }


def normalize(tokens, norm_gain):
    values = tokens.astype(jnp.float32)
    scale = lax.rsqrt(lax.optimization_barrier(jnp.mean(values * values, axis=-1, keepdims=True)) + 1e-06)
    return (values * scale * norm_gain[None, :]).astype(jnp.bfloat16)

def reference(tokens, norm_gain, chosen, route_weight, gate_weight, up_weight, down_weight):
    normed = normalize(tokens, norm_gain)

    def expert_step(combined, inputs):
        token_ids, weights, gate_mat, up_mat, down_mat = inputs
        expert_rows = normed[token_ids]
        gate_pre = jnp.dot(expert_rows, gate_mat, preferred_element_type=jnp.float32)
        up_pre = jnp.dot(expert_rows, up_mat, preferred_element_type=jnp.float32)
        hidden = (jax.nn.silu(gate_pre) * up_pre).astype(jnp.bfloat16)
        hidden_blocks = hidden.reshape(CAP, N_TP, FF_BLK).astype(jnp.float32)
        down_blocks = down_mat.reshape(N_TP, FF_BLK, D).astype(jnp.float32)
        partial_value = jnp.einsum('cnf,nfd->ncd', hidden_blocks, down_blocks).astype(jnp.bfloat16)
        partial_value = lax.optimization_barrier(partial_value)
        summed = lax.optimization_barrier(jnp.sum(partial_value.astype(jnp.float32), axis=0))
        weighted = (weights[:, None] * summed).astype(jnp.bfloat16)
        combined = combined.at[token_ids].add(weighted.astype(jnp.float32))
        return (combined, None)
    start_total = jnp.zeros((TOKENS, D), jnp.float32)
    combined, _ = lax.scan(expert_step, start_total, (chosen, route_weight, gate_weight, up_weight, down_weight))
    return combined.astype(jnp.bfloat16)
```

```python
import functools
import jax
import jax.numpy as jnp
from jax import lax
from jax.experimental import pallas as pl
from jax.experimental.pallas import tpu as pltpu
from jax.sharding import PartitionSpec as P

F32 = jnp.float32
BF16 = jnp.bfloat16
MESH = pl.DeviceIdType.MESH
PARTS = 2

def shards(tokens, norm_gain, chosen, route_weight, gate_weight, up_weight, down_weight):
    tok_rows, row_width = tokens.shape
    experts, capacity = chosen.shape
    ep_count = lax.axis_size("ep")
    tp_count = lax.axis_size("tp")
    owner_index = lax.axis_index("ep")
    slot_most = 3 * tok_rows // 16
    col_width = row_width // tp_count
    values = tokens.astype(jnp.float32)
    scale = lax.rsqrt(jnp.mean(values * values, axis=-1, keepdims=True) + 1e-06)
    normed = (values * scale * norm_gain[None, :]).astype(jnp.bfloat16)
    slot_steps = jnp.arange(slot_most, dtype=jnp.int32)
    first_token = owner_index * tok_rows
    run_start = jnp.sum((chosen < first_token).astype(jnp.int32), axis=1)
    run_end = jnp.sum((chosen < first_token + tok_rows).astype(jnp.int32), axis=1)
    run_count = run_end - run_start
    slot_live = slot_steps[None, :] < run_count[:, None]
    slot_place = jnp.minimum(run_start[:, None] + slot_steps[None, :], capacity - 1)
    slot_token = jnp.take_along_axis(chosen, slot_place, axis=1) - first_token
    slot_local = jnp.where(slot_live, slot_token, 0)
    my_chosen = lax.dynamic_index_in_dim(chosen, owner_index, 0, keepdims=False)
    block_edges = jnp.arange(ep_count, dtype=jnp.int32) * tok_rows
    src_start = jnp.sum((my_chosen[None, :] < block_edges[:, None]).astype(jnp.int32), axis=1)
    src_end = jnp.concatenate([src_start[1:], jnp.full((1,), capacity, jnp.int32)])
    gate_mat = gate_weight[0]
    up_mat = up_weight[0]
    down_mat = down_weight[0]
    outgoing = jnp.where(slot_live[:, :, None], normed[slot_local], jnp.zeros((), jnp.bfloat16))
    received = lax.all_to_all(outgoing, "ep", split_axis=0, concat_axis=0, tiled=True)
    source_block = my_chosen // tok_rows
    flat_index = (
        source_block * slot_most + jnp.arange(capacity, dtype=jnp.int32) - src_start[source_block]
    )
    expert_rows = received.reshape(-1, row_width)[flat_index]
    gate_pre = jnp.dot(expert_rows, gate_mat, preferred_element_type=jnp.float32)
    up_pre = jnp.dot(expert_rows, up_mat, preferred_element_type=jnp.float32)
    hidden = (jax.nn.silu(gate_pre) * up_pre).astype(jnp.bfloat16)
    summed_out = lax.psum_scatter(
        lax.dot_general(
            down_mat, hidden, (((0,), (1,)), ((), ())), preferred_element_type=jnp.float32
        ).astype(jnp.bfloat16),
        "tp",
        scatter_dimension=0,
        tiled=True,
    ).astype(jnp.float32)
    weighted = (summed_out.T * route_weight[0][:, None]).astype(jnp.bfloat16)
    back_place = jnp.minimum(src_start[:, None] + slot_steps[None, :], capacity - 1)
    back_live = slot_steps[None, :] < (src_end - src_start)[:, None]
    outgoing_back = jnp.where(
        back_live[:, :, None], weighted[back_place], jnp.zeros((), jnp.bfloat16)
    )
    returned = lax.all_to_all(outgoing_back, "ep", split_axis=0, concat_axis=0, tiled=True)
    target_row = jnp.where(slot_live, slot_token, tok_rows).reshape(-1)
    placement = (jnp.arange(tok_rows, dtype=jnp.int32)[:, None] == target_row[None, :]).astype(
        jnp.bfloat16
    )
    combined = jnp.dot(
        placement, returned.reshape(-1, col_width), preferred_element_type=jnp.float32
    )
    return combined.astype(jnp.bfloat16)


def fused_kernel(
    ep, nk, slots,
    tokens, gain, chosen, route, gate_hbm, up_hbm, down_hbm, out,
    gate_w, up_w, down_w, normed, pick, unpick, spread, gather, outgoing, received, rows, gate_acc,
    up_acc, hidden, pair_out, pair_in, own_part, cross_out, cross_in, back_out, back_in,
    w_sem, ep_send, ep_recv, y_send, y_recv, pair_send, pair_recv, relay_send, relay_recv,
    ps_send, ps_recv, ys_send, ys_recv, back_send, back_recv,
):
    me = lax.axis_index("ep")
    tp = lax.axis_index("tp")
    y_pos = tp // 2
    core = tp % 2
    mate = y_pos * 2 + (1 - core)
    across = (1 - y_pos) * 2 + core
    diag = (1 - y_pos) * 2 + (1 - core)
    tok_rows, width = tokens.shape
    cap = chosen.shape[1]
    quarter = width // 4
    piece = quarter // nk
    ff = gate_w.shape[1]
    order = [d for d in sorted(range(1, ep), key=lambda d: abs(d - ep / 2))]

    half = width // 2
    loads = []
    for i in range(2):
        part = pl.ds(i * half, half)
        loads.append(pltpu.make_async_copy(gate_hbm.at[0, part], gate_w.at[part], w_sem.at[3 * i]))
        loads.append(pltpu.make_async_copy(up_hbm.at[0, part], up_w.at[part], w_sem.at[3 * i + 1]))
    loads.append(pltpu.make_async_copy(down_hbm.at[0], down_w, w_sem.at[2]))
    for load in loads:
        load.start()

    barrier = pltpu.get_barrier_semaphore()
    for d in order:
        pl.semaphore_signal(
            barrier, inc=1, device_id={"ep": (me + d) % ep, "tp": tp}, device_id_type=MESH
        )
    for other in (mate, across):
        pl.semaphore_signal(barrier, inc=1, device_id={"ep": me, "tp": other}, device_id_type=MESH)

    my_cols = pl.ds(pl.multiple_of(tp * quarter, quarter), quarter)
    my_gain = gain[:, my_cols]
    step_rows = 32

    @pl.loop(0, tok_rows // step_rows)
    def _(r):
        rs = pl.ds(pl.multiple_of(r * step_rows, step_rows), step_rows)
        v = tokens[rs, :].astype(F32)
        scale = lax.rsqrt(jnp.sum(v * v, axis=1, keepdims=True) * (1.0 / width) + 1e-06)
        own = tokens[rs, my_cols].astype(F32)
        normed[rs, :] = (own * scale * my_gain).astype(BF16)

    first = me * tok_rows
    lane = lax.broadcasted_iota(jnp.int32, (slots, cap), 1).astype(F32)
    sub = lax.broadcasted_iota(jnp.int32, (slots, cap), 0).astype(F32)
    tok_lane = lax.broadcasted_iota(jnp.int32, (slots, tok_rows), 1).astype(F32)
    for e in range(ep):
        row = chosen[e : e + 1, :]
        local = (row - first).astype(F32)
        start = jnp.sum(jnp.where(local < 0.0, 1.0, 0.0), axis=1, keepdims=True)
        value = jnp.where((local >= 0.0) & (local < float(tok_rows)), local + 1.0, 0.0)
        hit = lane == sub + start
        slot_tok = jnp.sum(jnp.where(hit, value, 0.0), axis=1, keepdims=True) - 1.0
        pick[e * slots : (e + 1) * slots, :] = jnp.where(tok_lane == slot_tok, 1.0, 0.0)

    pick_b = pick[...].astype(BF16)
    for k in range(nk):
        got = jnp.dot(pick_b, normed[:, k * piece : (k + 1) * piece], preferred_element_type=F32)
        outgoing[k] = got.astype(BF16).reshape(ep, slots, piece)

    pl.semaphore_wait(barrier, ep + 1)

    def ep_copy(buf_out, buf_in, s_sem, r_sem, k, d):
        dest = (me + d) % ep
        return pltpu.make_async_remote_copy(
            src_ref=buf_out.at[k, dest], dst_ref=buf_in.at[k, me],
            send_sem=s_sem.at[k, d], recv_sem=r_sem.at[k, d],
            device_id={"ep": dest, "tp": tp}, device_id_type=MESH,
        )

    def tp_copy(a, b, s_sem, r_sem, k, other):
        return pltpu.make_async_remote_copy(
            src_ref=a, dst_ref=b, send_sem=s_sem.at[k], recv_sem=r_sem.at[k],
            device_id={"ep": me, "tp": other}, device_id_type=MESH,
        )

    sends = []
    dispatch = [[ep_copy(outgoing, received, ep_send, ep_recv, k, d) for d in order] for k in range(nk)]
    for k in range(nk):
        for c in dispatch[k]:
            c.start()
            sends.append(c)
    for k in range(nk):
        received[k, me] = outgoing[k, me]

    mine = chosen[pl.ds(me, 1), :].astype(F32)
    place = lax.broadcasted_iota(jnp.int32, (1, cap), 1).astype(F32)
    slot_id = jnp.zeros((1, cap), F32)
    for b in range(ep):
        lo = float(b * tok_rows)
        begin = jnp.sum(jnp.where(mine < lo, 1.0, 0.0), axis=1, keepdims=True)
        inside = (mine >= lo) & (mine < lo + float(tok_rows))
        slot_id = jnp.where(inside, place - begin + float(b * slots), slot_id)
    slot_sub = lax.broadcasted_iota(jnp.int32, (ep * slots, cap), 0).astype(F32)
    spread_f = jnp.where(slot_sub == slot_id, 1.0, 0.0)
    spread[...] = spread_f.astype(BF16)
    gather[...] = spread_f.T.astype(BF16)
    unpick[...] = pick[...].T.astype(BF16)
    eye_r = lax.broadcasted_iota(jnp.int32, (cap, cap), 0)
    eye_c = lax.broadcasted_iota(jnp.int32, (cap, cap), 1)
    weight = jnp.sum(jnp.where(eye_r == eye_c, route[...], 0.0), axis=1, keepdims=True)

    def compact(k):
        for c in dispatch[k]:
            c.wait_recv()
        got = jnp.dot(
            gather[...], received[k].reshape(ep * slots, piece), preferred_element_type=F32
        )
        rows[tp, k] = got.astype(BF16)
        for c in (
            tp_copy(rows.at[tp, k], rows.at[tp, k], y_send, y_recv, k, across),
            tp_copy(rows.at[tp, k], rows.at[tp, k], pair_send, pair_recv, k, mate),
        ):
            c.start()
            sends.append(c)

    def relay(k):
        tp_copy(rows.at[tp, k], rows.at[across, k], y_send, y_recv, k, across).wait_recv()
        c = tp_copy(rows.at[across, k], rows.at[across, k], relay_send, relay_recv, k, mate)
        c.start()
        sends.append(c)

    tile = 256

    def project(k):
        if k == 0:
            for load in loads[:4]:
                load.wait()
        tp_copy(rows.at[tp, k], rows.at[mate, k], pair_send, pair_recv, k, mate).wait_recv()
        tp_copy(rows.at[tp, k], rows.at[diag, k], relay_send, relay_recv, k, mate).wait_recv()

        @pl.loop(0, ff // tile)
        def _(n):
            cols = pl.ds(pl.multiple_of(n * tile, tile), tile)
            g = jnp.zeros((cap, tile), F32) if k == 0 else gate_acc[:, cols]
            u = jnp.zeros((cap, tile), F32) if k == 0 else up_acc[:, cols]
            for t in range(4):
                ks = slice(t * quarter + k * piece, t * quarter + (k + 1) * piece)
                x = rows[t, k]
                g = g + jnp.dot(x, gate_w[ks, cols], preferred_element_type=F32)
                u = u + jnp.dot(x, up_w[ks, cols], preferred_element_type=F32)
            if k < nk - 1:
                gate_acc[:, cols] = g
                up_acc[:, cols] = u
            else:
                hidden[:, cols] = (g / (1.0 + jnp.exp(-g)) * u).astype(BF16)

    for k in range(nk + 2):
        if k < nk:
            compact(k)
        if 1 <= k <= nk:
            relay(k - 1)
        if k >= 2:
            project(k - 2)
    loads[4].wait()

    def down(t, k):
        cols = pl.ds(pl.multiple_of(t * quarter + k * piece, piece), piece)
        return jnp.dot(hidden[...], down_w[:, cols], preferred_element_type=F32)

    other_y = 1 - y_pos
    pair_c = [tp_copy(pair_out.at[k], pair_in.at[k], ps_send, ps_recv, k, mate) for k in range(nk)]
    cross_c = [tp_copy(cross_out.at[k], cross_in.at[k], ys_send, ys_recv, k, across) for k in range(nk)]
    for k in range(nk):
        pair_out[k, 0] = down(diag, k).astype(BF16)
        pair_out[k, 1] = down(mate, k).astype(BF16)
        pair_c[k].start()
        away = down(across, k)
        own_part[k] = down(tp, k)
        pair_c[k].wait_recv()
        cross_out[k] = (away + pair_in[k, 0].astype(F32)).astype(BF16)
        cross_c[k].start()
    back = [[ep_copy(back_out, back_in, back_send, back_recv, k, d) for d in order] for k in range(nk)]
    for k in range(nk):
        near = own_part[k] + pair_in[k, 1].astype(F32)
        cross_c[k].wait_recv()
        total = (near + cross_in[k].astype(F32)) * weight
        wide = jnp.dot(spread[...], total.astype(BF16), preferred_element_type=F32)
        back_out[k] = wide.astype(BF16).reshape(ep, slots, piece)
        for c in back[k]:
            c.start()
            sends.append(c)
        back_in[k, me] = back_out[k, me]
    for k in range(nk):
        for c in back[k]:
            c.wait_recv()
        done = jnp.dot(
            unpick[...], back_in[k].reshape(ep * slots, piece), preferred_element_type=F32
        )
        out[:, k * piece : (k + 1) * piece] = done.astype(BF16)
    for c in sends + pair_c + cross_c:
        c.wait_send()


def fused(tokens, norm_gain, chosen, route_weight, gate_weight, up_weight, down_weight):
    ep = lax.axis_size("ep")
    nk = PARTS
    tok_rows, width = tokens.shape
    cap = chosen.shape[1]
    slots = 3 * tok_rows // 16
    quarter = width // lax.axis_size("tp")
    piece = quarter // nk
    ff = gate_weight.shape[2]
    vmem = pl.BlockSpec(memory_space=pltpu.VMEM)
    hbm = pl.BlockSpec(memory_space=pl.ANY)
    dma = pltpu.SemaphoreType.DMA
    slot_buf = pltpu.VMEM((nk, ep, slots, piece), BF16)
    return pl.pallas_call(
        functools.partial(fused_kernel, ep, nk, slots),
        out_shape=jax.ShapeDtypeStruct((tok_rows, quarter), BF16),
        in_specs=[vmem] * 4 + [hbm] * 3,
        out_specs=vmem,
        scratch_shapes=[
            pltpu.VMEM((width, ff), BF16),
            pltpu.VMEM((width, ff), BF16),
            pltpu.VMEM((ff, width), BF16),
            pltpu.VMEM((tok_rows, quarter), BF16),
            pltpu.VMEM((ep * slots, tok_rows), F32),
            pltpu.VMEM((tok_rows, ep * slots), BF16),
            pltpu.VMEM((ep * slots, cap), BF16),
            pltpu.VMEM((cap, ep * slots), BF16),
            slot_buf,
            slot_buf,
            pltpu.VMEM((4, nk, cap, piece), BF16),
            pltpu.VMEM((cap, ff), F32),
            pltpu.VMEM((cap, ff), F32),
            pltpu.VMEM((cap, ff), BF16),
            pltpu.VMEM((nk, 2, cap, piece), BF16),
            pltpu.VMEM((nk, 2, cap, piece), BF16),
            pltpu.VMEM((nk, cap, piece), F32),
            pltpu.VMEM((nk, cap, piece), BF16),
            pltpu.VMEM((nk, cap, piece), BF16),
            slot_buf,
            slot_buf,
            dma((6,)),
            dma((nk, ep)),
            dma((nk, ep)),
        ]
        + [dma((nk,))] * 10
        + [dma((nk, ep))] * 2,
        compiler_params=pltpu.CompilerParams(
            collective_id=0, has_side_effects=True, vmem_limit_bytes=48 * 1024 * 1024
        ),
    )(tokens, norm_gain[None, :], chosen, route_weight, gate_weight, up_weight, down_weight)


def solution(mesh):
    small = mesh.shape["tp"] == 4
    return jax.shard_map(
        fused if small else shards,
        mesh=mesh,
        in_specs=(
            P("ep", None),
            P(),
            P(),
            P("ep", None),
            P("ep", None, "tp"),
            P("ep", None, "tp"),
            P("ep", "tp", None),
        ),
        out_specs=P("ep", "tp"),
        check_vma=False,
    )
```

```python
import functools
import jax
import jax.numpy as jnp
from jax import lax
from jax.experimental import pallas as pl
from jax.experimental.pallas import tpu as pltpu
from jax.sharding import PartitionSpec as P

F32 = jnp.float32
BF16 = jnp.bfloat16
MESH = pl.DeviceIdType.MESH
CUTS_IN = (4, 2, 2)
CUTS_OUT = (2, 2, 4)

def shards(tokens, norm_gain, chosen, route_weight, gate_weight, up_weight, down_weight):
    tok_rows, row_width = tokens.shape
    experts, capacity = chosen.shape
    ep_count = lax.axis_size("ep")
    tp_count = lax.axis_size("tp")
    owner_index = lax.axis_index("ep")
    slot_most = 3 * tok_rows // 16
    col_width = row_width // tp_count
    values = tokens.astype(jnp.float32)
    scale = lax.rsqrt(jnp.mean(values * values, axis=-1, keepdims=True) + 1e-06)
    normed = (values * scale * norm_gain[None, :]).astype(jnp.bfloat16)
    slot_steps = jnp.arange(slot_most, dtype=jnp.int32)
    first_token = owner_index * tok_rows
    run_start = jnp.sum((chosen < first_token).astype(jnp.int32), axis=1)
    run_end = jnp.sum((chosen < first_token + tok_rows).astype(jnp.int32), axis=1)
    run_count = run_end - run_start
    slot_live = slot_steps[None, :] < run_count[:, None]
    slot_place = jnp.minimum(run_start[:, None] + slot_steps[None, :], capacity - 1)
    slot_token = jnp.take_along_axis(chosen, slot_place, axis=1) - first_token
    slot_local = jnp.where(slot_live, slot_token, 0)
    my_chosen = lax.dynamic_index_in_dim(chosen, owner_index, 0, keepdims=False)
    block_edges = jnp.arange(ep_count, dtype=jnp.int32) * tok_rows
    src_start = jnp.sum((my_chosen[None, :] < block_edges[:, None]).astype(jnp.int32), axis=1)
    src_end = jnp.concatenate([src_start[1:], jnp.full((1,), capacity, jnp.int32)])
    gate_mat = gate_weight[0]
    up_mat = up_weight[0]
    down_mat = down_weight[0]
    outgoing = jnp.where(slot_live[:, :, None], normed[slot_local], jnp.zeros((), jnp.bfloat16))
    received = lax.all_to_all(outgoing, "ep", split_axis=0, concat_axis=0, tiled=True)
    source_block = my_chosen // tok_rows
    flat_index = (
        source_block * slot_most + jnp.arange(capacity, dtype=jnp.int32) - src_start[source_block]
    )
    expert_rows = received.reshape(-1, row_width)[flat_index]
    gate_pre = jnp.dot(expert_rows, gate_mat, preferred_element_type=jnp.float32)
    up_pre = jnp.dot(expert_rows, up_mat, preferred_element_type=jnp.float32)
    hidden = (jax.nn.silu(gate_pre) * up_pre).astype(jnp.bfloat16)
    summed_out = lax.psum_scatter(
        lax.dot_general(
            down_mat, hidden, (((0,), (1,)), ((), ())), preferred_element_type=jnp.float32
        ).astype(jnp.bfloat16),
        "tp",
        scatter_dimension=0,
        tiled=True,
    ).astype(jnp.float32)
    weighted = (summed_out.T * route_weight[0][:, None]).astype(jnp.bfloat16)
    back_place = jnp.minimum(src_start[:, None] + slot_steps[None, :], capacity - 1)
    back_live = slot_steps[None, :] < (src_end - src_start)[:, None]
    outgoing_back = jnp.where(
        back_live[:, :, None], weighted[back_place], jnp.zeros((), jnp.bfloat16)
    )
    returned = lax.all_to_all(outgoing_back, "ep", split_axis=0, concat_axis=0, tiled=True)
    target_row = jnp.where(slot_live, slot_token, tok_rows).reshape(-1)
    placement = (jnp.arange(tok_rows, dtype=jnp.int32)[:, None] == target_row[None, :]).astype(
        jnp.bfloat16
    )
    combined = jnp.dot(
        placement, returned.reshape(-1, col_width), preferred_element_type=jnp.float32
    )
    return combined.astype(jnp.bfloat16)


def fused_kernel(
    ep, slots, cuts_in, cuts_out,
    tokens_hbm, gain_hbm, chosen_hbm, route_hbm, gate_hbm, up_hbm, down_hbm, out,
    tokens, gain, chosen, route,
    gate_w, up_w, down_w, normed, pick, unpick, spread, gather, gate_acc, up_acc, hidden,
    outgoing, received, rows, pair_out, pair_in, own_part, cross_out, cross_in, back_out, back_in,
    in_sem, w_sem, ep_send, ep_recv, y_send, y_recv, pair_send, pair_recv, relay_send, relay_recv,
    ps_send, ps_recv, ys_send, ys_recv, back_send, back_recv,
):
    me = lax.axis_index("ep")
    tp = lax.axis_index("tp")
    y_pos = tp // 2
    core = tp % 2
    mate = y_pos * 2 + (1 - core)
    across = (1 - y_pos) * 2 + core
    diag = (1 - y_pos) * 2 + (1 - core)
    tok_rows, width = tokens.shape
    cap = chosen.shape[1]
    quarter = width // 4
    ff = gate_w.shape[1]
    order = [d for d in sorted(range(1, ep), key=lambda d: abs(d - ep / 2))]

    barrier = pltpu.get_barrier_semaphore()
    for d in order:
        pl.semaphore_signal(
            barrier, inc=1, device_id={"ep": (me + d) % ep, "tp": tp}, device_id_type=MESH
        )
    for other in (mate, across):
        pl.semaphore_signal(barrier, inc=1, device_id={"ep": me, "tp": other}, device_id_type=MESH)

    small = [
        pltpu.make_async_copy(a, b, in_sem.at[i])
        for i, (a, b) in enumerate(
            [(tokens_hbm, tokens), (gain_hbm, gain), (chosen_hbm, chosen), (route_hbm, route)]
        )
    ]
    for load in small:
        load.start()
    half = width // 2
    loads = []
    for i in range(2):
        part = pl.ds(i * half, half)
        loads.append(pltpu.make_async_copy(gate_hbm.at[0, part], gate_w.at[part], w_sem.at[3 * i]))
        loads.append(pltpu.make_async_copy(up_hbm.at[0, part], up_w.at[part], w_sem.at[3 * i + 1]))
    loads.append(pltpu.make_async_copy(down_hbm.at[0], down_w, w_sem.at[2]))
    for load in loads:
        load.start()
    for load in small:
        load.wait()

    first = me * tok_rows
    lane = lax.broadcasted_iota(jnp.int32, (slots, cap), 1).astype(F32)
    sub = lax.broadcasted_iota(jnp.int32, (slots, cap), 0).astype(F32)
    tok_lane = lax.broadcasted_iota(jnp.int32, (slots, tok_rows), 1).astype(F32)
    for e in range(ep):
        row = chosen[e : e + 1, :]
        local = (row - first).astype(F32)
        start = jnp.sum(jnp.where(local < 0.0, 1.0, 0.0), axis=1, keepdims=True)
        value = jnp.where((local >= 0.0) & (local < float(tok_rows)), local + 1.0, 0.0)
        hit = lane == sub + start
        slot_tok = jnp.sum(jnp.where(hit, value, 0.0), axis=1, keepdims=True) - 1.0
        pick[e * slots : (e + 1) * slots, :] = jnp.where(tok_lane == slot_tok, 1.0, 0.0)

    my_cols = pl.ds(pl.multiple_of(tp * quarter, quarter), quarter)
    my_gain = gain[:, my_cols]
    step_rows = 32

    @pl.loop(0, tok_rows // step_rows)
    def _(r):
        rs = pl.ds(pl.multiple_of(r * step_rows, step_rows), step_rows)
        v = tokens[rs, :].astype(F32)
        scale = lax.rsqrt(jnp.sum(v * v, axis=1, keepdims=True) * (1.0 / width) + 1e-06)
        own = tokens[rs, my_cols].astype(F32)
        normed[rs, :] = (own * scale * my_gain).astype(BF16)

    pick_b = pick[...].astype(BF16)
    for k, (off, size) in enumerate(cuts_in):
        got = jnp.dot(pick_b, normed[:, off : off + size], preferred_element_type=F32)
        outgoing[k][...] = got.astype(BF16).reshape(ep, slots, size)

    pl.semaphore_wait(barrier, ep + 1)

    def ep_copy(buf_out, buf_in, s_sem, r_sem, k, d):
        dest = (me + d) % ep
        return pltpu.make_async_remote_copy(
            src_ref=buf_out[k].at[dest], dst_ref=buf_in[k].at[me],
            send_sem=s_sem.at[k, d], recv_sem=r_sem.at[k, d],
            device_id={"ep": dest, "tp": tp}, device_id_type=MESH,
        )

    def tp_copy(a, b, s_sem, r_sem, k, other):
        return pltpu.make_async_remote_copy(
            src_ref=a, dst_ref=b, send_sem=s_sem.at[k], recv_sem=r_sem.at[k],
            device_id={"ep": me, "tp": other}, device_id_type=MESH,
        )

    sends = []

    def go(c):
        c.start()
        sends.append(c)

    n_in = len(cuts_in)
    dispatch = [
        [ep_copy(outgoing, received, ep_send, ep_recv, k, d) for d in order] for k in range(n_in)
    ]
    for k in range(n_in):
        for c in dispatch[k]:
            go(c)
    for k in range(n_in):
        received[k][me] = outgoing[k][me]

    mine = chosen[pl.ds(me, 1), :].astype(F32)
    place = lax.broadcasted_iota(jnp.int32, (1, cap), 1).astype(F32)
    slot_id = jnp.zeros((1, cap), F32)
    for b in range(ep):
        lo = float(b * tok_rows)
        begin = jnp.sum(jnp.where(mine < lo, 1.0, 0.0), axis=1, keepdims=True)
        inside = (mine >= lo) & (mine < lo + float(tok_rows))
        slot_id = jnp.where(inside, place - begin + float(b * slots), slot_id)
    slot_sub = lax.broadcasted_iota(jnp.int32, (ep * slots, cap), 0).astype(F32)
    spread_f = jnp.where(slot_sub == slot_id, 1.0, 0.0)
    spread[...] = spread_f.astype(BF16)
    gather[...] = spread_f.T.astype(BF16)
    unpick[...] = pick[...].T.astype(BF16)
    eye_r = lax.broadcasted_iota(jnp.int32, (cap, cap), 0)
    eye_c = lax.broadcasted_iota(jnp.int32, (cap, cap), 1)
    weight = jnp.sum(jnp.where(eye_r == eye_c, route[...], 0.0), axis=1, keepdims=True)

    def compact(k):
        size = cuts_in[k][1]
        for c in dispatch[k]:
            c.wait_recv()
        got = jnp.dot(
            gather[...], received[k][...].reshape(ep * slots, size), preferred_element_type=F32
        )
        mine_k = rows[k].at[tp]
        mine_k[...] = got.astype(BF16)
        go(tp_copy(mine_k, mine_k, y_send, y_recv, k, across))
        go(tp_copy(mine_k, mine_k, pair_send, pair_recv, k, mate))

    def relay(k):
        there = rows[k].at[across]
        tp_copy(rows[k].at[tp], there, y_send, y_recv, k, across).wait_recv()
        go(tp_copy(there, there, relay_send, relay_recv, k, mate))

    def project(near, far, opening=False, closing=False):
        for k in near:
            tp_copy(rows[k].at[tp], rows[k].at[mate], pair_send, pair_recv, k, mate).wait_recv()
        for k in far:
            tp_copy(rows[k].at[tp], rows[k].at[diag], relay_send, relay_recv, k, mate).wait_recv()
        work = [(k, t) for k in near for t in (tp, mate)] + [(k, t) for k in far for t in (across, diag)]
        tile = 256

        @pl.loop(0, ff // tile)
        def _(n):
            cols = pl.ds(pl.multiple_of(n * tile, tile), tile)
            g = None if opening else gate_acc[:, cols]
            u = None if opening else up_acc[:, cols]
            for k, t in work:
                off, size = cuts_in[k]
                ks = pl.ds(pl.multiple_of(t * quarter + off, 128), size)
                x = rows[k][t]
                dg = jnp.dot(x, gate_w[ks, cols], preferred_element_type=F32)
                du = jnp.dot(x, up_w[ks, cols], preferred_element_type=F32)
                g = dg if g is None else g + dg
                u = du if u is None else u + du
            if closing:
                hidden[:, cols] = (g / (1.0 + jnp.exp(-g)) * u).astype(BF16)
            else:
                gate_acc[:, cols] = g
                up_acc[:, cols] = u

    compact(0)
    compact(1)
    for load in loads[:4]:
        load.wait()
    project([0], [], opening=True)
    compact(2)
    relay(0)
    relay(1)
    project([1], [0])
    relay(2)
    project([2], [1])
    project([], [2], closing=True)
    loads[4].wait()

    def down(t, k):
        off, size = cuts_out[k]
        cols = pl.ds(pl.multiple_of(t * quarter + off, 128), size)
        return jnp.dot(hidden[...], down_w[:, cols], preferred_element_type=F32)

    n_out = len(cuts_out)
    pair_c = [tp_copy(pair_out[k], pair_in[k], ps_send, ps_recv, k, mate) for k in range(n_out)]
    cross_c = [tp_copy(cross_out[k], cross_in[k], ys_send, ys_recv, k, across) for k in range(n_out)]
    back = [
        [ep_copy(back_out, back_in, back_send, back_recv, k, d) for d in order] for k in range(n_out)
    ]

    def give(k):
        pair_out[k][0] = down(diag, k).astype(BF16)
        pair_out[k][1] = down(mate, k).astype(BF16)
        go(pair_c[k])

    def keep(k):
        own_part[k][0] = down(across, k)
        own_part[k][1] = down(tp, k)

    def cross(k):
        pair_c[k].wait_recv()
        cross_out[k][...] = (own_part[k][0] + pair_in[k][0].astype(F32)).astype(BF16)
        go(cross_c[k])

    def back_send_all(k):
        size = cuts_out[k][1]
        near = own_part[k][1] + pair_in[k][1].astype(F32)
        cross_c[k].wait_recv()
        total = (near + cross_in[k][...].astype(F32)) * weight
        wide = jnp.dot(spread[...], total.astype(BF16), preferred_element_type=F32)
        back_out[k][...] = wide.astype(BF16).reshape(ep, slots, size)
        for c in back[k]:
            go(c)
        back_in[k][me] = back_out[k][me]

    give(0)
    keep(0)
    for k in range(1, n_out):
        give(k)
        cross(k - 1)
        keep(k)
    cross(n_out - 1)
    for k in range(n_out):
        back_send_all(k)
    for k, (off, size) in enumerate(cuts_out):
        for c in back[k]:
            c.wait_recv()
        done = jnp.dot(
            unpick[...], back_in[k][...].reshape(ep * slots, size), preferred_element_type=F32
        )
        out[:, off : off + size] = done.astype(BF16)
    for c in sends:
        c.wait_send()


def cut(quarter, eighths):
    sizes = [quarter * e // 8 for e in eighths]
    return [(sum(sizes[:i]), size) for i, size in enumerate(sizes)]


def fused(tokens, norm_gain, chosen, route_weight, gate_weight, up_weight, down_weight):
    ep = lax.axis_size("ep")
    tok_rows, width = tokens.shape
    cap = chosen.shape[1]
    slots = 3 * tok_rows // 16
    quarter = width // lax.axis_size("tp")
    ff = gate_weight.shape[2]
    cuts_in = cut(quarter, CUTS_IN)
    cuts_out = cut(quarter, CUTS_OUT)
    hbm = pl.BlockSpec(memory_space=pl.ANY)
    dma = pltpu.SemaphoreType.DMA

    def bufs(cuts, lead, dtype=BF16):
        return [pltpu.VMEM(lead + (size,), dtype) for _, size in cuts]

    n_in, n_out = len(cuts_in), len(cuts_out)
    return pl.pallas_call(
        functools.partial(fused_kernel, ep, slots, cuts_in, cuts_out),
        out_shape=jax.ShapeDtypeStruct((tok_rows, quarter), BF16),
        in_specs=[hbm] * 7,
        out_specs=pl.BlockSpec(memory_space=pltpu.VMEM),
        scratch_shapes=[
            pltpu.VMEM((tok_rows, width), BF16),
            pltpu.VMEM((1, width), F32),
            pltpu.VMEM(chosen.shape, jnp.int32),
            pltpu.VMEM((1, cap), F32),
            pltpu.VMEM((width, ff), BF16),
            pltpu.VMEM((width, ff), BF16),
            pltpu.VMEM((ff, width), BF16),
            pltpu.VMEM((tok_rows, quarter), BF16),
            pltpu.VMEM((ep * slots, tok_rows), F32),
            pltpu.VMEM((tok_rows, ep * slots), BF16),
            pltpu.VMEM((ep * slots, cap), BF16),
            pltpu.VMEM((cap, ep * slots), BF16),
            pltpu.VMEM((cap, ff), F32),
            pltpu.VMEM((cap, ff), F32),
            pltpu.VMEM((cap, ff), BF16),
            bufs(cuts_in, (ep, slots)),
            bufs(cuts_in, (ep, slots)),
            bufs(cuts_in, (4, cap)),
            bufs(cuts_out, (2, cap)),
            bufs(cuts_out, (2, cap)),
            bufs(cuts_out, (2, cap), F32),
            bufs(cuts_out, (cap,)),
            bufs(cuts_out, (cap,)),
            bufs(cuts_out, (ep, slots)),
            bufs(cuts_out, (ep, slots)),
            dma((4,)),
            dma((5,)),
            dma((n_in, ep)),
            dma((n_in, ep)),
        ]
        + [dma((n_in,))] * 6
        + [dma((n_out,))] * 4
        + [dma((n_out, ep))] * 2,
        compiler_params=pltpu.CompilerParams(
            collective_id=0, has_side_effects=True, vmem_limit_bytes=60 * 1024 * 1024
        ),
    )(tokens, norm_gain[None, :], chosen, route_weight, gate_weight, up_weight, down_weight)


def solution(mesh):
    small = mesh.shape["tp"] == 4
    return jax.shard_map(
        fused if small else shards,
        mesh=mesh,
        in_specs=(
            P("ep", None),
            P(),
            P(),
            P("ep", None),
            P("ep", None, "tp"),
            P("ep", None, "tp"),
            P("ep", "tp", None),
        ),
        out_specs=P("ep", "tp"),
        check_vma=False,
    )
```

```python
import functools
import jax
import jax.numpy as jnp
from jax import lax
from jax.experimental import pallas as pl
from jax.experimental.pallas import tpu as pltpu
from jax.sharding import PartitionSpec as P

F32 = jnp.float32
BF16 = jnp.bfloat16
MESH = pl.DeviceIdType.MESH
CUTS_IN = (2, 4, 2)
CUTS_OUT = (2, 2, 4)

def shards(tokens, norm_gain, chosen, route_weight, gate_weight, up_weight, down_weight):
    tok_rows, row_width = tokens.shape
    experts, capacity = chosen.shape
    ep_count = lax.axis_size("ep")
    tp_count = lax.axis_size("tp")
    owner_index = lax.axis_index("ep")
    slot_most = 3 * tok_rows // 16
    col_width = row_width // tp_count
    values = tokens.astype(jnp.float32)
    scale = lax.rsqrt(jnp.mean(values * values, axis=-1, keepdims=True) + 1e-06)
    normed = (values * scale * norm_gain[None, :]).astype(jnp.bfloat16)
    slot_steps = jnp.arange(slot_most, dtype=jnp.int32)
    first_token = owner_index * tok_rows
    run_start = jnp.sum((chosen < first_token).astype(jnp.int32), axis=1)
    run_end = jnp.sum((chosen < first_token + tok_rows).astype(jnp.int32), axis=1)
    run_count = run_end - run_start
    slot_live = slot_steps[None, :] < run_count[:, None]
    slot_place = jnp.minimum(run_start[:, None] + slot_steps[None, :], capacity - 1)
    slot_token = jnp.take_along_axis(chosen, slot_place, axis=1) - first_token
    slot_local = jnp.where(slot_live, slot_token, 0)
    my_chosen = lax.dynamic_index_in_dim(chosen, owner_index, 0, keepdims=False)
    block_edges = jnp.arange(ep_count, dtype=jnp.int32) * tok_rows
    src_start = jnp.sum((my_chosen[None, :] < block_edges[:, None]).astype(jnp.int32), axis=1)
    src_end = jnp.concatenate([src_start[1:], jnp.full((1,), capacity, jnp.int32)])
    gate_mat = gate_weight[0]
    up_mat = up_weight[0]
    down_mat = down_weight[0]
    outgoing = jnp.where(slot_live[:, :, None], normed[slot_local], jnp.zeros((), jnp.bfloat16))
    received = lax.all_to_all(outgoing, "ep", split_axis=0, concat_axis=0, tiled=True)
    source_block = my_chosen // tok_rows
    flat_index = (
        source_block * slot_most + jnp.arange(capacity, dtype=jnp.int32) - src_start[source_block]
    )
    expert_rows = received.reshape(-1, row_width)[flat_index]
    gate_pre = jnp.dot(expert_rows, gate_mat, preferred_element_type=jnp.float32)
    up_pre = jnp.dot(expert_rows, up_mat, preferred_element_type=jnp.float32)
    hidden = (jax.nn.silu(gate_pre) * up_pre).astype(jnp.bfloat16)
    summed_out = lax.psum_scatter(
        lax.dot_general(
            down_mat, hidden, (((0,), (1,)), ((), ())), preferred_element_type=jnp.float32
        ).astype(jnp.bfloat16),
        "tp",
        scatter_dimension=0,
        tiled=True,
    ).astype(jnp.float32)
    weighted = (summed_out.T * route_weight[0][:, None]).astype(jnp.bfloat16)
    back_place = jnp.minimum(src_start[:, None] + slot_steps[None, :], capacity - 1)
    back_live = slot_steps[None, :] < (src_end - src_start)[:, None]
    outgoing_back = jnp.where(
        back_live[:, :, None], weighted[back_place], jnp.zeros((), jnp.bfloat16)
    )
    returned = lax.all_to_all(outgoing_back, "ep", split_axis=0, concat_axis=0, tiled=True)
    target_row = jnp.where(slot_live, slot_token, tok_rows).reshape(-1)
    placement = (jnp.arange(tok_rows, dtype=jnp.int32)[:, None] == target_row[None, :]).astype(
        jnp.bfloat16
    )
    combined = jnp.dot(
        placement, returned.reshape(-1, col_width), preferred_element_type=jnp.float32
    )
    return combined.astype(jnp.bfloat16)


def fused_kernel(
    ep, slots, cuts_in, cuts_out,
    tokens_hbm, gain_hbm, chosen_hbm, route_hbm, gate_hbm, up_hbm, down_hbm, out,
    tokens, gain, chosen, route,
    gate_w, up_w, down_w, normed, pick, unpick, spread, gather, gate_acc, up_acc, hidden,
    outgoing, received, rows, pair_out, pair_in, own_part, cross_out, cross_in, back_out, back_in,
    in_sem, w_sem, ep_send, ep_recv, y_send, y_recv, pair_send, pair_recv, relay_send, relay_recv,
    ps_send, ps_recv, ys_send, ys_recv, back_send, back_recv,
):
    me = lax.axis_index("ep")
    tp = lax.axis_index("tp")
    y_pos = tp // 2
    core = tp % 2
    mate = y_pos * 2 + (1 - core)
    across = (1 - y_pos) * 2 + core
    diag = (1 - y_pos) * 2 + (1 - core)
    tok_rows, width = tokens.shape
    cap = chosen.shape[1]
    quarter = width // 4
    ff = gate_w.shape[1]
    order = [d for d in sorted(range(1, ep), key=lambda d: abs(d - ep / 2))]

    barrier = pltpu.get_barrier_semaphore()
    for d in order:
        pl.semaphore_signal(
            barrier, inc=1, device_id={"ep": (me + d) % ep, "tp": tp}, device_id_type=MESH
        )
    for other in (mate, across):
        pl.semaphore_signal(barrier, inc=1, device_id={"ep": me, "tp": other}, device_id_type=MESH)

    small = [
        pltpu.make_async_copy(a, b, in_sem.at[i])
        for i, (a, b) in enumerate(
            [(tokens_hbm, tokens), (gain_hbm, gain), (chosen_hbm, chosen), (route_hbm, route)]
        )
    ]
    for load in (small[2], small[0], small[1], small[3]):
        load.start()
    half = width // 2
    loads = []
    for i in range(2):
        part = pl.ds(i * half, half)
        loads.append(pltpu.make_async_copy(gate_hbm.at[0, part], gate_w.at[part], w_sem.at[3 * i]))
        loads.append(pltpu.make_async_copy(up_hbm.at[0, part], up_w.at[part], w_sem.at[3 * i + 1]))
    loads.append(pltpu.make_async_copy(down_hbm.at[0], down_w, w_sem.at[2]))
    for load in small[2:]:
        load.wait()

    first = me * tok_rows
    lane = lax.broadcasted_iota(jnp.int32, (slots, cap), 1).astype(F32)
    sub = lax.broadcasted_iota(jnp.int32, (slots, cap), 0).astype(F32)
    tok_lane = lax.broadcasted_iota(jnp.int32, (slots, tok_rows), 1).astype(F32)
    for e in range(ep):
        row = chosen[e : e + 1, :]
        local = (row - first).astype(F32)
        start = jnp.sum(jnp.where(local < 0.0, 1.0, 0.0), axis=1, keepdims=True)
        value = jnp.where((local >= 0.0) & (local < float(tok_rows)), local + 1.0, 0.0)
        hit = lane == sub + start
        slot_tok = jnp.sum(jnp.where(hit, value, 0.0), axis=1, keepdims=True) - 1.0
        pick[e * slots : (e + 1) * slots, :] = jnp.where(tok_lane == slot_tok, 1.0, 0.0)

    pick_b = pick[...].astype(BF16)
    for load in small[:2]:
        load.wait()

    my_cols = pl.ds(pl.multiple_of(tp * quarter, quarter), quarter)
    my_gain = gain[:, my_cols]
    step_rows = 32

    @pl.loop(0, tok_rows // step_rows)
    def _(r):
        rs = pl.ds(pl.multiple_of(r * step_rows, step_rows), step_rows)
        v = tokens[rs, :].astype(F32)
        scale = lax.rsqrt(jnp.sum(v * v, axis=1, keepdims=True) * (1.0 / width) + 1e-06)
        own = tokens[rs, my_cols].astype(F32)
        normed[rs, :] = (own * scale * my_gain).astype(BF16)

    for k, (off, size) in enumerate(cuts_in):
        got = jnp.dot(pick_b, normed[:, off : off + size], preferred_element_type=F32)
        outgoing[k][...] = got.astype(BF16).reshape(ep, slots, size)

    pl.semaphore_wait(barrier, ep + 1)

    def ep_copy(buf_out, buf_in, s_sem, r_sem, k, d):
        dest = (me + d) % ep
        return pltpu.make_async_remote_copy(
            src_ref=buf_out[k].at[dest], dst_ref=buf_in[k].at[me],
            send_sem=s_sem.at[k, d], recv_sem=r_sem.at[k, d],
            device_id={"ep": dest, "tp": tp}, device_id_type=MESH,
        )

    def tp_copy(a, b, s_sem, r_sem, k, other):
        return pltpu.make_async_remote_copy(
            src_ref=a, dst_ref=b, send_sem=s_sem.at[k], recv_sem=r_sem.at[k],
            device_id={"ep": me, "tp": other}, device_id_type=MESH,
        )

    sends = []

    def go(c):
        c.start()
        sends.append(c)

    n_in = len(cuts_in)
    dispatch = [
        [ep_copy(outgoing, received, ep_send, ep_recv, k, d) for d in order] for k in range(n_in)
    ]
    for k in range(n_in):
        for c in dispatch[k]:
            go(c)
    for load in loads:
        load.start()
    for k in range(n_in):
        received[k][me] = outgoing[k][me]

    mine = chosen[pl.ds(me, 1), :].astype(F32)
    place = lax.broadcasted_iota(jnp.int32, (1, cap), 1).astype(F32)
    slot_id = jnp.zeros((1, cap), F32)
    for b in range(ep):
        lo = float(b * tok_rows)
        begin = jnp.sum(jnp.where(mine < lo, 1.0, 0.0), axis=1, keepdims=True)
        inside = (mine >= lo) & (mine < lo + float(tok_rows))
        slot_id = jnp.where(inside, place - begin + float(b * slots), slot_id)
    slot_sub = lax.broadcasted_iota(jnp.int32, (ep * slots, cap), 0).astype(F32)
    spread_f = jnp.where(slot_sub == slot_id, 1.0, 0.0)
    spread[...] = spread_f.astype(BF16)
    gather[...] = spread_f.T.astype(BF16)
    unpick[...] = pick[...].T.astype(BF16)
    eye_r = lax.broadcasted_iota(jnp.int32, (cap, cap), 0)
    eye_c = lax.broadcasted_iota(jnp.int32, (cap, cap), 1)
    weight = jnp.sum(jnp.where(eye_r == eye_c, route[...], 0.0), axis=1, keepdims=True)

    def compact(k):
        size = cuts_in[k][1]
        for c in dispatch[k]:
            c.wait_recv()
        got = jnp.dot(
            gather[...], received[k][...].reshape(ep * slots, size), preferred_element_type=F32
        )
        mine_k = rows[k].at[tp]
        mine_k[...] = got.astype(BF16)
        go(tp_copy(mine_k, mine_k, y_send, y_recv, k, across))
        go(tp_copy(mine_k, mine_k, pair_send, pair_recv, k, mate))

    def relay(k):
        there = rows[k].at[across]
        tp_copy(rows[k].at[tp], there, y_send, y_recv, k, across).wait_recv()
        go(tp_copy(there, there, relay_send, relay_recv, k, mate))

    def project(near, far, opening=False, closing=False):
        for k in near:
            tp_copy(rows[k].at[tp], rows[k].at[mate], pair_send, pair_recv, k, mate).wait_recv()
        for k in far:
            tp_copy(rows[k].at[tp], rows[k].at[diag], relay_send, relay_recv, k, mate).wait_recv()
        work = [(k, t) for k in near for t in (tp, mate)] + [(k, t) for k in far for t in (across, diag)]
        tile = 256

        @pl.loop(0, ff // tile)
        def _(n):
            cols = pl.ds(pl.multiple_of(n * tile, tile), tile)
            g = None if opening else gate_acc[:, cols]
            u = None if opening else up_acc[:, cols]
            for k, t in work:
                off, size = cuts_in[k]
                ks = pl.ds(pl.multiple_of(t * quarter + off, 128), size)
                x = rows[k][t]
                dg = jnp.dot(x, gate_w[ks, cols], preferred_element_type=F32)
                du = jnp.dot(x, up_w[ks, cols], preferred_element_type=F32)
                g = dg if g is None else g + dg
                u = du if u is None else u + du
            if closing:
                hidden[:, cols] = (g / (1.0 + jnp.exp(-g)) * u).astype(BF16)
            else:
                gate_acc[:, cols] = g
                up_acc[:, cols] = u

    compact(0)
    compact(1)
    for load in loads[:4]:
        load.wait()
    project([0], [], opening=True)
    compact(2)
    relay(0)
    relay(1)
    project([1], [0])
    relay(2)
    project([2], [1])
    project([], [2], closing=True)
    loads[4].wait()

    def down(t, k):
        off, size = cuts_out[k]
        cols = pl.ds(pl.multiple_of(t * quarter + off, 128), size)
        return jnp.dot(hidden[...], down_w[:, cols], preferred_element_type=F32)

    n_out = len(cuts_out)
    pair_c = [tp_copy(pair_out[k], pair_in[k], ps_send, ps_recv, k, mate) for k in range(n_out)]
    cross_c = [tp_copy(cross_out[k], cross_in[k], ys_send, ys_recv, k, across) for k in range(n_out)]
    back = [
        [ep_copy(back_out, back_in, back_send, back_recv, k, d) for d in order] for k in range(n_out)
    ]

    def give(k):
        pair_out[k][0] = down(diag, k).astype(BF16)
        pair_out[k][1] = down(mate, k).astype(BF16)
        go(pair_c[k])

    def keep(k):
        own_part[k][0] = down(across, k)
        own_part[k][1] = down(tp, k)

    def cross(k):
        pair_c[k].wait_recv()
        cross_out[k][...] = (own_part[k][0] + pair_in[k][0].astype(F32)).astype(BF16)
        go(cross_c[k])

    def back_send_all(k):
        size = cuts_out[k][1]
        near = own_part[k][1] + pair_in[k][1].astype(F32)
        cross_c[k].wait_recv()
        total = (near + cross_in[k][...].astype(F32)) * weight
        wide = jnp.dot(spread[...], total.astype(BF16), preferred_element_type=F32)
        back_out[k][...] = wide.astype(BF16).reshape(ep, slots, size)
        for c in back[k]:
            go(c)
        back_in[k][me] = back_out[k][me]

    give(0)
    keep(0)
    for k in range(1, n_out):
        give(k)
        cross(k - 1)
        keep(k)
    cross(n_out - 1)
    for k in range(n_out):
        back_send_all(k)
    for k, (off, size) in enumerate(cuts_out):
        for c in back[k]:
            c.wait_recv()
        done = jnp.dot(
            unpick[...], back_in[k][...].reshape(ep * slots, size), preferred_element_type=F32
        )
        out[:, off : off + size] = done.astype(BF16)
    for c in sends:
        c.wait_send()


def cut(quarter, eighths):
    sizes = [quarter * e // 8 for e in eighths]
    return [(sum(sizes[:i]), size) for i, size in enumerate(sizes)]


def fused(tokens, norm_gain, chosen, route_weight, gate_weight, up_weight, down_weight):
    ep = lax.axis_size("ep")
    tok_rows, width = tokens.shape
    cap = chosen.shape[1]
    slots = 3 * tok_rows // 16
    quarter = width // lax.axis_size("tp")
    ff = gate_weight.shape[2]
    cuts_in = cut(quarter, CUTS_IN)
    cuts_out = cut(quarter, CUTS_OUT)
    hbm = pl.BlockSpec(memory_space=pl.ANY)
    dma = pltpu.SemaphoreType.DMA

    def bufs(cuts, lead, dtype=BF16):
        return [pltpu.VMEM(lead + (size,), dtype) for _, size in cuts]

    n_in, n_out = len(cuts_in), len(cuts_out)
    return pl.pallas_call(
        functools.partial(fused_kernel, ep, slots, cuts_in, cuts_out),
        out_shape=jax.ShapeDtypeStruct((tok_rows, quarter), BF16),
        in_specs=[hbm] * 7,
        out_specs=pl.BlockSpec(memory_space=pltpu.VMEM),
        scratch_shapes=[
            pltpu.VMEM((tok_rows, width), BF16),
            pltpu.VMEM((1, width), F32),
            pltpu.VMEM(chosen.shape, jnp.int32),
            pltpu.VMEM((1, cap), F32),
            pltpu.VMEM((width, ff), BF16),
            pltpu.VMEM((width, ff), BF16),
            pltpu.VMEM((ff, width), BF16),
            pltpu.VMEM((tok_rows, quarter), BF16),
            pltpu.VMEM((ep * slots, tok_rows), F32),
            pltpu.VMEM((tok_rows, ep * slots), BF16),
            pltpu.VMEM((ep * slots, cap), BF16),
            pltpu.VMEM((cap, ep * slots), BF16),
            pltpu.VMEM((cap, ff), F32),
            pltpu.VMEM((cap, ff), F32),
            pltpu.VMEM((cap, ff), BF16),
            bufs(cuts_in, (ep, slots)),
            bufs(cuts_in, (ep, slots)),
            bufs(cuts_in, (4, cap)),
            bufs(cuts_out, (2, cap)),
            bufs(cuts_out, (2, cap)),
            bufs(cuts_out, (2, cap), F32),
            bufs(cuts_out, (cap,)),
            bufs(cuts_out, (cap,)),
            bufs(cuts_out, (ep, slots)),
            bufs(cuts_out, (ep, slots)),
            dma((4,)),
            dma((5,)),
            dma((n_in, ep)),
            dma((n_in, ep)),
        ]
        + [dma((n_in,))] * 6
        + [dma((n_out,))] * 4
        + [dma((n_out, ep))] * 2,
        compiler_params=pltpu.CompilerParams(
            collective_id=0, has_side_effects=True, vmem_limit_bytes=60 * 1024 * 1024
        ),
    )(tokens, norm_gain[None, :], chosen, route_weight, gate_weight, up_weight, down_weight)


def solution(mesh):
    small = mesh.shape["tp"] == 4
    return jax.shard_map(
        fused if small else shards,
        mesh=mesh,
        in_specs=(
            P("ep", None),
            P(),
            P(),
            P("ep", None),
            P("ep", None, "tp"),
            P("ep", None, "tp"),
            P("ep", "tp", None),
        ),
        out_specs=P("ep", "tp"),
        check_vma=False,
    )
```
